32 devices in a mesh: sp: 8 (over z, x), tp: 4 (over y, core).
Axes of the slice: x: 2, y: 2, z: 4, core: 2. Of those that a mesh axis runs over, the one named last changes fastest.
Arguments:
- cotangent: bfloat16 [1536, 2048], P('sp'), may hold values from -8 to 8
- residual: bfloat16 [1536, 2048], P('sp'), may hold values from -6 to 6
- norm_gain: float32 [2048], replicated, may hold values from 0.1 to 1.9
- route_ids: int32 [1536, 2], P('sp'), may hold values from 0 to 7, all different within a row; in each aligned block of 192 rows (0 to 191, 192 to 383, ...) at most 96 rows name the same one
- route_weights: float32 [1536, 2], P('sp'), may hold values from 0.1 to 1
- expert_gate: bfloat16 [8, 2048, 1024], P('sp', None, 'tp'), may hold values from -0.125 to 0.125
- expert_up: bfloat16 [8, 2048, 1024], P('sp', None, 'tp'), may hold values from -0.125 to 0.125
- expert_down: bfloat16 [8, 1024, 2048], P('sp', 'tp'), may hold values from -0.1875 to 0.1875
- out_proj: bfloat16 [2048, 1024], P(None, 'tp'), may hold values from -0.1875 to 0.1875
- conv_out: bfloat16 [1536, 1024], P('sp', 'tp'), may hold values from -6 to 6, as said below
- branch_gate: bfloat16 [1536, 1024], P('sp', 'tp'), may hold values from -6 to 6
- prev_state: bfloat16 [1536, 1024], P('sp', 'tp'), may hold values from -6 to 6
- decay_param: float32 [1024], P('tp'), as said below
- rate_map: bfloat16 [16, 64, 64], P('tp'), may hold values from -0.75 to 0.75
- input_map: bfloat16 [16, 64, 64], P('tp'), may hold values from -0.75 to 0.75
Outputs:
- grad_gate: float32 [8, 2048, 1024], P('sp', None, 'tp')
- grad_up: float32 [8, 2048, 1024], P('sp', None, 'tp')
- grad_down: float32 [8, 1024, 2048], P('sp', 'tp')
- grad_out_proj: float32 [2048, 1024], P('sp', 'tp')
- grad_conv_out: float32 [1536, 1024], P('sp', 'tp')
- grad_branch_gate: float32 [1536, 1024], P('sp', 'tp')
The draws below stay inside these ranges and needn't reach their ends.
Inputs may be any that keep to these rules, and one draw needn't show every extreme that they name: `route_ids`: within the rows of one device (aligned blocks of 192 rows) no expert is named by more than 96 rows, a bound that some block reaches; the two ids of a row differ. `conv_out`: every entry is a finite value between -6 and 6. `decay_param`: every channel's decay parameter is at least 4.
All inputs are finite; a program needn't handle non-finite values.
Results may differ from the reference program's by a relative error of at most 0.0095.
Values may be sent and summed in bfloat16 or wider, within the bound.
No kernel may reach another device: no remote copies, remote signals or barrier semaphores. Data moves between devices by JAX's collectives and lax.ppermute only.
A program may use at most 128 MiB of HBM per device.

```python
import math
import jax
import jax.numpy as jnp
import numpy as np
from jax import lax

D = 2048
FF = 1024
W = 1024
LRU_BLOCK = 64
TOK_DEV = 192
EXPERTS = 8
CAP = 96
TOKENS = 1536
FF_PART = 256
BLOCKS = 16
N_SP = 8
N_TP = 4


def draw_conv_out(key, part):
    noise_key, offset_key = jax.random.split(key, 2)
    offsets = jax.random.uniform(offset_key, (TOKENS // 64,), jnp.float32, -1.5, 1.5)
    shifts = jnp.repeat(offsets, 64)[:, None]
    base_values = jax.random.normal(noise_key, (TOKENS, W), jnp.float32)
    return jnp.clip(base_values + shifts, -6.0, 6.0).astype(jnp.bfloat16)


def draw_decay_param(key, part):
    pick_key, slow_key, fast_key = jax.random.split(key, 3)
    chooser = jax.random.uniform(pick_key, (W,), jnp.float32)
    slow_values = jnp.log(TOKENS * 1.0) + jax.random.uniform(slow_key, (W,), jnp.float32, 1.5, 3.0)
    fast_values = jax.random.uniform(fast_key, (W,), jnp.float32, 4.8, 6.0)
    slow_share = 0.5
    return jnp.where(chooser < slow_share, slow_values, fast_values).astype(jnp.float32)


def spiked(drawn, own_key, source, target, shards_of, factor):
    def block_of(position):
        return (jnp.arange(drawn.shape[position]) // (drawn.shape[position] // shards_of)).reshape((-1,) + (1,) * (drawn.ndim - 1 - position))

    near = jax.random.permutation(own_key, shards_of)[block_of(target)]
    second = (block_of(target) + shards_of // 2) % shards_of
    return jnp.where((block_of(source) == near) | (block_of(source) == second), factor * drawn, drawn)


def block_scale(own_key, dims, cuts, smallest, high):
    level = 1.0
    for axis_at, shards_of in cuts:
        heights = jax.random.uniform(jax.random.fold_in(jax.random.fold_in(own_key, 6), axis_at), (shards_of,), jnp.float32, smallest / len(cuts), high / len(cuts))
        level = level * jnp.repeat(jnp.exp(heights), dims[axis_at] // shards_of).reshape((-1,) + (1,) * (len(dims) - 1 - axis_at))
    return level


def assign_block(own_key, own, number, rows, number_of, top, limit, skew):
    order = jax.random.permutation(own_key, number_of)
    crowded, common = portions_of(number_of, rows * top, limit, skew, True), portions_of(number_of, rows * top, limit, skew, False)
    places = jnp.arange(number_of)

    def named(sizes, rotation):
        used = int((sizes > 0).sum())
        fixed = max(1, used // 4)
        moved = fixed + (places - fixed + rotation * (used - fixed)) % max(1, number_of - fixed)
        return jnp.zeros((number_of,), jnp.int32).at[order[jnp.where(places < fixed, places, moved)]].set(jnp.asarray(sizes, jnp.int32))

    sizes = jnp.where(number % 4 == 0, named(crowded, number // 4), named(common, number - number // 4 - 1))
    mixed = jax.random.permutation(jax.random.fold_in(own, 3), number_of)
    giver, receiver = mixed[0:number_of // 2 * 2:2], mixed[1:number_of // 2 * 2:2]
    margin = jnp.minimum(sizes[giver] - 1, limit - sizes[receiver]) // 2
    margin = jnp.where((giver == order[0]) | (receiver == order[0]) | (sizes[receiver] == 0), 0, jnp.maximum(margin, 0))
    moved = jax.random.randint(jax.random.fold_in(own, 4), (number_of // 2,), 0, 1 << 20) % (margin + 1)
    sizes = sizes.at[giver].add(-moved).at[receiver].add(moved)
    labels = jnp.searchsorted(jnp.cumsum(sizes), jnp.arange(rows * top), side="right").astype(jnp.int32)
    listing = labels.reshape(top, rows).T
    listing = listing[jax.random.permutation(jax.random.fold_in(own, 1), rows)]
    rotation = jax.random.randint(jax.random.fold_in(own, 2), (rows, 1), 0, top)
    return jnp.take_along_axis(listing, (jnp.arange(top)[None, :] + rotation) % top, axis=1)


def portions_of(amount, total, limit, skew, full):
    portions = [(1 << 20) // math.isqrt(rank ** skew) + 1 for rank in range(1, amount + 1)]
    largest = limit if full else min(limit, max(-(-total // amount), total * portions[0] // sum(portions)))
    least = 1 if total - largest >= amount - 1 else 0
    holding, surplus = [largest] + [least] * (amount - 1), total - largest - least * (amount - 1)
    while surplus > 0:
        movable = [i for i in range(1, amount) if holding[i] < largest] or [i for i in range(1, amount) if holding[i] < limit]
        pool, left = sum([portions[i] for i in movable]), surplus
        for i in movable:
            extra = min(limit - holding[i], max(1, left * portions[i] // pool), surplus)
            holding[i] = holding[i] + extra
            surplus = surplus - extra
    return np.array(holding)


def centred(key, extent, scale, bound, shards=(), kind=jnp.bfloat16):
    loudness = block_scale(key, extent, shards, -0.22, 0.18) if shards else 1.0
    array = jax.random.normal(key, extent, jnp.float32) * scale * loudness
    return jnp.minimum(jnp.maximum(array, -bound), bound).astype(kind)


def gaussian_with(stream_key, extent, scale, limit, cuts, heavy, held_as=jnp.bfloat16):
    drawn = scale * jax.random.normal(stream_key, extent, jnp.float32)
    if cuts:
        drawn = drawn * block_scale(stream_key, extent, cuts, -0.22, 0.18)
    return jnp.clip(spiked(drawn, jax.random.fold_in(stream_key, 3), *heavy), -limit, limit).astype(held_as)


def setup_inputs(seed: int = 0) -> dict:
    streams_of = jax.random.split(jax.random.key(seed), 16)
    cotangent = gaussian_with(streams_of[0], (TOKENS, D), 1.0, 8.0, ((0, 8),), (0, 1, 8, 2.0))
    residual = centred(streams_of[1], (TOKENS, D), 1.0, 6.0, ((0, 8),))
    norm_gain = jnp.clip(1.0 + 0.18 * jax.random.normal(streams_of[2], (D,), jnp.float32), 0.1, 1.9)
    route_ids_keys = jax.random.split(jax.random.fold_in(streams_of[3], 1), TOKENS // TOK_DEV)
    route_ids_turns = jax.random.permutation(jax.random.fold_in(streams_of[3], 3), TOKENS // TOK_DEV)
    route_ids = jax.vmap(lambda own, number: assign_block(jax.random.fold_in(streams_of[3], 2), own, number, TOK_DEV, EXPERTS, 2, CAP, 1))(route_ids_keys, route_ids_turns).reshape((TOKENS, 2))
    route_weights = jnp.clip(0.1 + 0.9 * jax.random.uniform(streams_of[4], (TOKENS, 2), jnp.float32) ** block_scale(streams_of[4], (TOKENS, 2), ((0, 8),), -0.2, 0.2), 0.1, 1.0)
    expert_gate = centred(streams_of[5], (EXPERTS, D, FF), D ** -0.5, 0.125, ((0, 8), (2, 4)))
    expert_up = centred(streams_of[6], (EXPERTS, D, FF), D ** -0.5, 0.125, ((0, 8), (2, 4)))
    expert_down = centred(streams_of[7], (EXPERTS, FF, D), FF ** -0.5, 0.1875, ((0, 8), (1, 4)))
    out_proj = centred(streams_of[8], (D, W), W ** -0.5, 0.1875, ((1, 4),))
    conv_out = draw_conv_out(jax.random.fold_in(streams_of[15], 71), 0)
    branch_gate = centred(streams_of[10], (TOKENS, W), 1.0, 6.0, ((0, 8), (1, 4)))
    prev_state = centred(streams_of[11], (TOKENS, W), 1.0, 6.0, ((0, 8), (1, 4)))
    decay_param = draw_decay_param(jax.random.fold_in(streams_of[15], 71), 0)
    rate_map = centred(streams_of[13], (BLOCKS, LRU_BLOCK, LRU_BLOCK), LRU_BLOCK ** -0.5, 0.75, ((0, 4),))
    input_map = centred(streams_of[14], (BLOCKS, LRU_BLOCK, LRU_BLOCK), LRU_BLOCK ** -0.5, 0.75, ((0, 4),))
    return {"cotangent": cotangent, "residual": residual, "norm_gain": norm_gain, "route_ids": route_ids, "route_weights": route_weights, "expert_gate": expert_gate, "expert_up": expert_up, "expert_down": expert_down, "out_proj": out_proj, "conv_out": conv_out, "branch_gate": branch_gate, "prev_state": prev_state, "decay_param": decay_param, "rate_map": rate_map, "input_map": input_map}


RATE_SCALE = 8.0
NORM_EPS = 1e-06
SERIES_EDGE = 0.001

def gelu_pair(values):
    result, pullback = jax.vjp(jax.nn.gelu, values)
    return (result, pullback(jnp.ones_like(values))[0])

def gate_maps(conv_out, weights):
    rows_here = conv_out.shape[0]
    blocked = conv_out.astype(jnp.float32).reshape(rows_here, weights.shape[0], weights.shape[1])
    mapped = jnp.einsum('tbi,bij->tbj', blocked, weights.astype(jnp.float32))
    return mapped.reshape(rows_here, -1)

def gate_maps_back(grad_values, weights):
    rows_here = grad_values.shape[0]
    blocked = grad_values.reshape(rows_here, weights.shape[0], weights.shape[2])
    mapped = jnp.einsum('tbj,bij->tbi', blocked, weights.astype(jnp.float32), precision=lax.Precision.HIGHEST)
    return mapped.reshape(rows_here, -1)

def norm_slope(spread):
    tiny_side = spread < SERIES_EDGE
    denominator = jnp.where(tiny_side, 1.0, -jnp.expm1(-spread))
    series_ratio = jnp.where(tiny_side, 1.0 + 0.5 * spread, spread / denominator)
    return 0.5 * jnp.sqrt(spread * series_ratio)

def reverse_linear(factors, term_values):

    def combine(left_pair, right_pair):
        return (left_pair[0] * right_pair[0], right_pair[0] * left_pair[1] + right_pair[1])
    flipped = lax.associative_scan(combine, (jnp.flip(factors, 0), jnp.flip(term_values, 0)), axis=0)
    return jnp.flip(flipped[1], 0)

def reference(cotangent, residual, norm_gain, route_ids, route_weights, expert_gate, expert_up, expert_down, out_proj, conv_out, branch_gate, prev_state, decay_param, rate_map, input_map):
    res_values = residual.astype(jnp.float32)
    inv_rms = lax.rsqrt(lax.optimization_barrier(jnp.mean(res_values * res_values, axis=1, keepdims=True)) + NORM_EPS)
    moe_input = (res_values * inv_rms * norm_gain[None, :]).astype(jnp.bfloat16)
    scaled_cot = (route_weights[:, :, None] * cotangent.astype(jnp.float32)[:, None, :]).astype(jnp.bfloat16)
    scaled_cot = scaled_cot.reshape(2 * TOKENS, D)
    id_blocks = route_ids.reshape(N_SP, 2 * TOK_DEV)
    expert_hits = (id_blocks[:, :, None] == jnp.arange(EXPERTS, dtype=jnp.int32)[None, None, :]).astype(jnp.int32)
    earlier_hits = jnp.cumsum(expert_hits, axis=1) - expert_hits
    rank_in = lax.optimization_barrier(jnp.sum(earlier_hits * expert_hits, axis=2))
    global_slot = (id_blocks * (N_SP * CAP) + jnp.arange(N_SP, dtype=jnp.int32)[:, None] * CAP + rank_in).reshape(-1).astype(jnp.int32)
    slot_total = EXPERTS * N_SP * CAP
    assign_table = jnp.zeros((slot_total,), jnp.int32).at[global_slot].set(jnp.arange(2 * TOKENS, dtype=jnp.int32)).reshape(EXPERTS, N_SP * CAP)
    filled_table = jnp.zeros((slot_total,), jnp.int32).at[global_slot].set(1).reshape(EXPERTS, N_SP * CAP)

    def one_expert(packed):
        gate_one, up_one, down_one, assign_one, filled_one = packed
        rows_in = moe_input[assign_one // 2]
        cot_in = jnp.where(filled_one[:, None] > 0, scaled_cot[assign_one], jnp.zeros((), jnp.bfloat16))
        gate_pre = jnp.dot(rows_in, gate_one, preferred_element_type=jnp.float32)
        up_pre = jnp.dot(rows_in, up_one, preferred_element_type=jnp.float32)
        gate_sig = jax.nn.sigmoid(gate_pre)
        gate_act = gate_pre * gate_sig
        hidden = (gate_act * up_pre).astype(jnp.bfloat16)
        d_hidden = jnp.dot(cot_in, down_one.T, preferred_element_type=jnp.float32)
        d_up = (d_hidden * gate_act).astype(jnp.bfloat16)
        d_gate = (d_hidden * up_pre * gate_sig * (1.0 + gate_pre * (1.0 - gate_sig))).astype(jnp.bfloat16)
        grad_down_one = jnp.dot(hidden.T, cot_in, preferred_element_type=jnp.float32)
        grad_gate_one = jnp.dot(rows_in.T, d_gate, preferred_element_type=jnp.float32)
        grad_up_one = jnp.dot(rows_in.T, d_up, preferred_element_type=jnp.float32)
        rows_count = rows_in.shape[0]
        gate_blocks = d_gate.astype(jnp.float32).reshape(rows_count, N_TP, FF_PART)
        up_blocks = d_up.astype(jnp.float32).reshape(rows_count, N_TP, FF_PART)
        block_terms = jnp.einsum('rnf,dnf->nrd', gate_blocks, gate_one.astype(jnp.float32).reshape(D, N_TP, FF_PART))
        block_terms = block_terms + jnp.einsum('rnf,dnf->nrd', up_blocks, up_one.astype(jnp.float32).reshape(D, N_TP, FF_PART))
        rounded = lax.optimization_barrier(block_terms.astype(jnp.bfloat16))
        expert_back_one = lax.optimization_barrier(jnp.sum(rounded.astype(jnp.float32), axis=0)).astype(jnp.bfloat16)
        return (grad_gate_one, grad_up_one, grad_down_one, expert_back_one)
    grad_gate, grad_up, grad_down, expert_back = lax.map(one_expert, (expert_gate, expert_up, expert_down, assign_table, filled_table))
    back_rows = expert_back.reshape(slot_total, D)[global_slot].astype(jnp.float32)
    d_normed = lax.optimization_barrier(jnp.sum(back_rows.reshape(TOKENS, 2, D), axis=1))
    weighted = norm_gain[None, :] * d_normed
    cubed = inv_rms * inv_rms * inv_rms
    d_mix = (cotangent.astype(jnp.float32) + inv_rms * weighted - res_values * cubed * lax.optimization_barrier(jnp.mean(res_values * weighted, axis=1, keepdims=True))).astype(jnp.bfloat16)
    rate_gate = jax.nn.sigmoid(gate_maps(conv_out, rate_map))
    input_gate = jax.nn.sigmoid(gate_maps(conv_out, input_map))
    soft_decay = jax.nn.softplus(-decay_param)
    log_keep = -RATE_SCALE * rate_gate * soft_decay[None, :]
    keep_rate = jnp.exp(log_keep)
    spread = -2.0 * log_keep
    norm_term = jnp.sqrt(-jnp.expm1(-spread))
    conv_values = conv_out.astype(jnp.float32)
    prev_values = prev_state.astype(jnp.float32)
    state_now = keep_rate * prev_values + norm_term * input_gate * conv_values
    gelu_value, gelu_slope = gelu_pair(branch_gate.astype(jnp.float32))
    branch_out = (state_now * gelu_value).astype(jnp.bfloat16)
    grad_out_proj = lax.dot_general(d_mix, branch_out, (((0,), (0,)), ((), ())), preferred_element_type=jnp.float32)
    d_branch = jnp.dot(d_mix, out_proj, preferred_element_type=jnp.float32)
    next_keep = jnp.concatenate([keep_rate[1:], jnp.zeros_like(keep_rate[:1])], axis=0)
    state_grad = reverse_linear(next_keep, d_branch * gelu_value)
    grad_branch_gate = d_branch * state_now * gelu_slope
    keep_grad = state_grad * prev_values * keep_rate
    inner_input = input_gate * conv_values
    rate_back = keep_grad * (-RATE_SCALE * soft_decay[None, :]) * rate_gate * (1.0 - rate_gate)
    rate_back = rate_back + state_grad * inner_input * keep_rate * keep_rate * (1.0 - rate_gate) * norm_slope(spread)
    input_back = state_grad * norm_term * conv_values * input_gate * (1.0 - input_gate)
    grad_conv_out = state_grad * norm_term * input_gate + gate_maps_back(rate_back, rate_map) + gate_maps_back(input_back, input_map)
    return (grad_gate, grad_up, grad_down, grad_out_proj, grad_conv_out, grad_branch_gate)
```

```python
import jax
import jax.numpy as jnp
from jax import lax
from jax.sharding import PartitionSpec as P

RATE_SCALE = 8.0
NORM_EPS = 1e-06
SERIES_EDGE = 0.001


DIRECT_LIMIT = 8


def bits_of(count):
    return [1 << b for b in reversed(range(count.bit_length() - 1))]


def swap_by(x, axis, bit):
    count = lax.axis_size(axis)
    return lax.ppermute(x, axis, [(k, k ^ bit) for k in range(count)])


def is_direct(count):
    return count <= DIRECT_LIMIT and count & (count - 1) == 0


def exchange(stacked, axis):
    count = lax.axis_size(axis)
    if not is_direct(count):
        return lax.all_to_all(stacked, axis, split_axis=0, concat_axis=0, tiled=True)
    return jnp.stack([stacked[0]] + [swap_by(stacked[j], axis, j) for j in range(1, count)])


def collect(x, axis):
    count = lax.axis_size(axis)
    if not is_direct(count):
        return lax.all_gather(x, axis)
    return jnp.stack([x] + [swap_by(x, axis, j) for j in range(1, count)])


def xor_order(blocks, place):
    for bit in bits_of(len(blocks)):
        flip = (place & bit) != 0
        blocks = [jnp.where(flip, blocks[q ^ bit], blocks[q]) for q in range(len(blocks))]
    return blocks


def share_all(x, axis):
    count = lax.axis_size(axis)
    held = {0: x}
    for bit in bits_of(count):
        held.update({q ^ bit: swap_by(held[q], axis, bit) for q in list(held)})
    return [held[q] for q in range(count)]


def columns(x, count, dim):
    return jnp.split(x, count, axis=dim)


def from_later(keep_all, head, axis):
    count = lax.axis_size(axis)

    def shift(x, d):
        return lax.ppermute(x, axis, [(k, k - d) for k in range(d, count)])

    keep_span = shift(keep_all, 1)
    carry = shift(head, 1)
    d = 1
    while d < count:
        carry = carry + keep_span * shift(carry, d)
        if 2 * d < count:
            keep_span = keep_span * shift(keep_span, d)
        d *= 2
    return carry


def gelu_pair(values):
    result, pullback = jax.vjp(jax.nn.gelu, values)
    return (result, pullback(jnp.ones_like(values))[0])


def gate_maps(conv_out, weights):
    rows_here = conv_out.shape[0]
    blocked = conv_out.reshape(rows_here, weights.shape[0], weights.shape[1])
    mapped = jnp.einsum("tbi,bij->tbj", blocked, weights, preferred_element_type=jnp.float32)
    return mapped.reshape(rows_here, -1)


def gate_maps_back(grad_values, weights):
    rows_here = grad_values.shape[0]
    blocked = grad_values.reshape(rows_here, weights.shape[0], weights.shape[2])
    mapped = jnp.einsum(
        "tbj,bij->tbi", blocked, weights.astype(jnp.float32), precision=lax.Precision.HIGHEST
    )
    return mapped.reshape(rows_here, -1)


def norm_slope(spread):
    tiny_side = spread < SERIES_EDGE
    denominator = jnp.where(tiny_side, 1.0, -jnp.expm1(-spread))
    series_ratio = jnp.where(tiny_side, 1.0 + 0.5 * spread, spread / denominator)
    return 0.5 * jnp.sqrt(spread * series_ratio)


def reverse_linear(factors, term_values):

    def combine(left_pair, right_pair):
        return (left_pair[0] * right_pair[0], right_pair[0] * left_pair[1] + right_pair[1])

    flipped = lax.associative_scan(
        combine, (jnp.flip(factors, 0), jnp.flip(term_values, 0)), axis=0
    )
    return jnp.flip(flipped[1], 0)


def per_device(
    cotangent,
    residual,
    norm_gain,
    route_ids,
    route_weights,
    expert_gate,
    expert_up,
    expert_down,
    out_proj,
    conv_out,
    branch_gate,
    prev_state,
    decay_param,
    rate_map,
    input_map,
):
    tok_rows, model_width = residual.shape
    sp_count = lax.axis_size("sp")
    tp_count = lax.axis_size("tp")
    local_experts = expert_gate.shape[0]
    experts_all = local_experts * sp_count
    capacity = 4 * tok_rows // experts_all
    slot_total = experts_all * capacity
    sp_place = lax.axis_index("sp")
    tp_place = lax.axis_index("tp")
    part_cols = model_width // tp_count
    res_values = residual.astype(jnp.float32)
    inv_rms = lax.rsqrt(jnp.mean(res_values * res_values, axis=1, keepdims=True) + NORM_EPS)
    owner = jnp.arange(sp_count, dtype=jnp.int32)
    if is_direct(sp_count):
        owner = owner ^ sp_place
    expert_of = (
        owner[:, None] * local_experts + jnp.arange(local_experts, dtype=jnp.int32)[None, :]
    ).reshape(experts_all, 1)
    hits0 = expert_of == route_ids[:, 0][None, :]
    hits1 = expert_of == route_ids[:, 1][None, :]
    hits = hits0 | hits1
    before = jnp.arange(tok_rows)[:, None] < jnp.arange(tok_rows)[None, :]
    rank = jnp.dot(
        hits.astype(jnp.bfloat16), before.astype(jnp.bfloat16), preferred_element_type=jnp.float32
    ).astype(jnp.int32)
    slot_rank = jnp.where(hits, rank, -1)
    pick_mask = slot_rank[:, None, :] == jnp.arange(capacity, dtype=jnp.int32)[None, :, None]
    pick = pick_mask.astype(jnp.bfloat16).reshape(slot_total, tok_rows)
    pair_weight = jnp.where(hits0, route_weights[:, 0][None, :], route_weights[:, 1][None, :])
    slot_weight = jnp.sum(jnp.where(pick_mask, pair_weight[:, None, :], 0.0), axis=2).reshape(
        slot_total, 1
    )
    col_start = tp_place * part_cols
    res_part = lax.dynamic_slice_in_dim(residual, col_start, part_cols, 1).astype(jnp.float32)
    gain_part = lax.dynamic_slice_in_dim(norm_gain, col_start, part_cols, 0)
    rows_own = (res_part * inv_rms * gain_part[None, :]).astype(jnp.bfloat16)
    cot_own = lax.dynamic_slice_in_dim(cotangent, col_start, part_cols, 1)
    rows_send = jnp.dot(pick, rows_own, preferred_element_type=jnp.float32).astype(jnp.bfloat16)
    cot_send = (
        jnp.dot(pick, cot_own, preferred_element_type=jnp.float32) * slot_weight
    ).astype(jnp.bfloat16)

    def dispatch(rows):
        blocks = exchange(rows.reshape(sp_count, local_experts, capacity, part_cols), "sp")
        blocks = jnp.transpose(blocks, (1, 0, 2, 3))
        blocks = blocks.reshape(local_experts, sp_count * capacity, part_cols)
        return share_all(blocks, "tp")

    rows_in = dispatch(rows_send)
    cot_in = dispatch(cot_send)
    gate_w = xor_order(columns(expert_gate, tp_count, 1), tp_place)
    up_w = xor_order(columns(expert_up, tp_count, 1), tp_place)
    down_w = xor_order(columns(expert_down, tp_count, 2), tp_place)

    def total(form, lefts, rights):
        out = None
        for one, other in zip(lefts, rights):
            term = jnp.einsum(form, one, other, preferred_element_type=jnp.float32)
            out = term if out is None else out + term
        return out

    gate_pre = total("erd,edf->erf", rows_in, gate_w)
    up_pre = total("erd,edf->erf", rows_in, up_w)
    gate_sig = jax.nn.sigmoid(gate_pre)
    gate_act = gate_pre * gate_sig
    hidden = (gate_act * up_pre).astype(jnp.bfloat16)
    d_hidden = total("erd,efd->erf", cot_in, down_w)
    d_up = (d_hidden * gate_act).astype(jnp.bfloat16)
    d_gate = (d_hidden * up_pre * gate_sig * (1.0 + gate_pre * (1.0 - gate_sig))).astype(
        jnp.bfloat16
    )

    def back_term(q):
        return jnp.einsum(
            "erf,edf->erd", d_gate, gate_w[q], preferred_element_type=jnp.float32
        ) + jnp.einsum("erf,edf->erd", d_up, up_w[q], preferred_element_type=jnp.float32)

    back = {q: back_term(q) for q in reversed(range(tp_count))}
    for bit in reversed(bits_of(tp_count)):
        keep = [q for q in back if not q & bit]
        back = {
            q: back[q] + swap_by(back[q ^ bit].astype(jnp.bfloat16), "tp", bit).astype(jnp.float32)
            for q in keep
        }
    summed = back[0].astype(jnp.bfloat16)
    summed = jnp.transpose(
        summed.reshape(local_experts, sp_count, capacity, part_cols), (1, 0, 2, 3)
    )
    returned = exchange(summed, "sp").reshape(slot_total, part_cols)
    normed_part = lax.dot_general(
        pick, returned, (((0,), (0,)), ((), ())), preferred_element_type=jnp.float32
    )
    d_normed = jnp.concatenate(
        xor_order(share_all(normed_part.astype(jnp.bfloat16), "tp"), tp_place), axis=1
    ).astype(jnp.float32)

    def outer(form, lefts, rights, dim):
        parts = [
            jnp.einsum(form, one, other, preferred_element_type=jnp.float32)
            for one, other in zip(lefts, rights)
        ]
        return jnp.concatenate(xor_order(parts, tp_place), axis=dim)

    grad_down = outer("erf,erd->efd", [hidden] * tp_count, cot_in, 2)
    grad_gate = outer("erd,erf->edf", rows_in, [d_gate] * tp_count, 1)
    grad_up = outer("erd,erf->edf", rows_in, [d_up] * tp_count, 1)
    weighted = norm_gain[None, :] * d_normed
    cubed = inv_rms * inv_rms * inv_rms
    d_mix = (
        cotangent.astype(jnp.float32)
        + inv_rms * weighted
        - res_values * cubed * jnp.mean(res_values * weighted, axis=1, keepdims=True)
    ).astype(jnp.bfloat16)
    rate_gate = jax.nn.sigmoid(gate_maps(conv_out, rate_map))
    input_gate = jax.nn.sigmoid(gate_maps(conv_out, input_map))
    soft_decay = jax.nn.softplus(-decay_param)
    log_keep = -RATE_SCALE * rate_gate * soft_decay[None, :]
    keep_rate = jnp.exp(log_keep)
    spread = -2.0 * log_keep
    norm_term = jnp.sqrt(-jnp.expm1(-spread))
    conv_values = conv_out.astype(jnp.float32)
    prev_values = prev_state.astype(jnp.float32)
    state_now = keep_rate * prev_values + norm_term * input_gate * conv_values
    gelu_value, gelu_slope = gelu_pair(branch_gate.astype(jnp.float32))
    branch_out = (state_now * gelu_value).astype(jnp.bfloat16)
    branch_out, _ = lax.optimization_barrier((branch_out, cot_in[0][:, :8, :128]))
    branch_all = collect(branch_out, "sp")
    mix_parts = columns(d_mix, sp_count, 1)
    if is_direct(sp_count):
        mix_parts = xor_order(mix_parts, sp_place)
    mix_all = exchange(jnp.stack(mix_parts), "sp")
    grad_out_proj = lax.dot_general(
        mix_all.reshape(sp_count * tok_rows, -1),
        branch_all.reshape(sp_count * tok_rows, -1),
        (((0,), (0,)), ((), ())),
        preferred_element_type=jnp.float32,
    )
    d_branch = jnp.dot(d_mix, out_proj, preferred_element_type=jnp.float32)
    next_keep = jnp.concatenate([keep_rate[1:], jnp.zeros_like(keep_rate[:1])], axis=0)
    local_grad = reverse_linear(next_keep, d_branch * gelu_value)
    next_log = jnp.concatenate([log_keep[1:], jnp.zeros_like(log_keep[:1])], axis=0)
    tail_keep = jnp.exp(jnp.flip(jnp.cumsum(jnp.flip(next_log, 0), axis=0), 0))
    block_keep = jnp.exp(jnp.sum(log_keep, axis=0))
    head_term = keep_rate[0] * local_grad[0]

    carried = from_later(block_keep, head_term, "sp")
    state_grad = local_grad + tail_keep * carried[None, :]
    grad_branch_gate = d_branch * state_now * gelu_slope
    keep_grad = state_grad * prev_values * keep_rate
    inner_input = input_gate * conv_values
    rate_back = keep_grad * (-RATE_SCALE * soft_decay[None, :]) * rate_gate * (1.0 - rate_gate)
    rate_back = rate_back + state_grad * inner_input * keep_rate * keep_rate * (
        1.0 - rate_gate
    ) * norm_slope(spread)
    input_back = state_grad * norm_term * conv_values * input_gate * (1.0 - input_gate)
    grad_conv_out = (
        state_grad * norm_term * input_gate
        + gate_maps_back(rate_back, rate_map)
        + gate_maps_back(input_back, input_map)
    )
    return (grad_gate, grad_up, grad_down, grad_out_proj, grad_conv_out, grad_branch_gate)


def solution(mesh):
    in_specs = (
        P("sp", None),
        P("sp", None),
        P(),
        P("sp", None),
        P("sp", None),
        P("sp", None, "tp"),
        P("sp", None, "tp"),
        P("sp", "tp", None),
        P(None, "tp"),
        P("sp", "tp"),
        P("sp", "tp"),
        P("sp", "tp"),
        P("tp"),
        P("tp", None, None),
        P("tp", None, None),
    )
    out_specs = (
        P("sp", None, "tp"),
        P("sp", None, "tp"),
        P("sp", "tp", None),
        P("sp", "tp"),
        P("sp", "tp"),
        P("sp", "tp"),
    )
    return jax.shard_map(
        per_device, mesh=mesh, in_specs=in_specs, out_specs=out_specs, check_vma=False
    )
```

```python
import jax
import jax.numpy as jnp
from jax import lax
from jax.experimental import pallas as pl
from jax.experimental.pallas import tpu as pltpu
from jax.sharding import PartitionSpec as P

RATE_SCALE = 8.0
NORM_EPS = 1e-06
SERIES_EDGE = 0.001


DIRECT_LIMIT = 8


def bits_of(count):
    return [1 << b for b in reversed(range(count.bit_length() - 1))]


def swap_by(x, axis, bit):
    count = lax.axis_size(axis)
    return lax.ppermute(x, axis, [(k, k ^ bit) for k in range(count)])


def is_direct(count):
    return count <= DIRECT_LIMIT and count & (count - 1) == 0


def join(blocks):
    count = len(blocks)
    shape = blocks[0].shape

    def kernel(*refs):
        for j in range(count):
            refs[count][j] = refs[j][...]

    return pl.pallas_call(
        kernel, out_shape=jax.ShapeDtypeStruct((count,) + shape, blocks[0].dtype), name="join"
    )(*blocks)


def exchange(stacked, axis):
    count = lax.axis_size(axis)
    if not is_direct(count):
        return lax.all_to_all(stacked, axis, split_axis=0, concat_axis=0, tiled=True)
    return join([stacked[0]] + [swap_by(stacked[j], axis, j) for j in range(1, count)])


def three_pieces(x):
    first = lax.reduce_precision(x, 8, 7)
    second = lax.reduce_precision(x - first, 8, 7)
    third = x - first - second
    return jnp.stack([first, second, third]).astype(jnp.bfloat16)


def sum_pieces(rows):
    rows = rows.astype(jnp.float32)
    return rows[0] + rows[1] + rows[2]


def with_tail(x, pieces, rows):
    pad = jnp.zeros((rows - pieces.shape[0], x.shape[1]), x.dtype)
    return jnp.concatenate([x, pieces, pad], axis=0)


def deal_columns(x, tail, place, count):
    rows, width = x.shape
    cols = width // count

    def kernel(place_ref, x_ref, tail_ref, *outs):
        for j in range(count):
            start = pl.multiple_of((place_ref[0] ^ j) * cols, cols)
            outs[j][:rows] = x_ref[:, pl.ds(start, cols)]
            outs[j][rows:] = tail_ref[...]

    shape = jax.ShapeDtypeStruct((rows + tail.shape[0], cols), x.dtype)
    vmem = pl.BlockSpec(memory_space=pltpu.VMEM)
    return pl.pallas_call(
        kernel,
        out_shape=[shape] * count,
        in_specs=[pl.BlockSpec(memory_space=pltpu.SMEM), vmem, vmem],
        out_specs=[vmem] * count,
        name="deal",
    )(place.reshape(1).astype(jnp.int32), x, tail)


def sum_outer(lefts, rights, rows):
    count = len(lefts)

    def kernel(*refs):
        total = None
        for j in range(count):
            term = lax.dot_general(
                refs[j][:rows],
                refs[count + j][:rows],
                (((0,), (0,)), ((), ())),
                preferred_element_type=jnp.float32,
            )
            total = term if total is None else total + term
        refs[2 * count][...] = total

    shape = (lefts[0].shape[1], rights[0].shape[1])
    return pl.pallas_call(
        kernel, out_shape=jax.ShapeDtypeStruct(shape, jnp.float32), name="sum_outer"
    )(*lefts, *rights)


def later_factors(spans, place):
    run = jnp.ones_like(spans[0])
    factors = []
    for k, one in enumerate(spans):
        later = k > place
        factors.append(jnp.where(later, run, 0.0))
        run = jnp.where(later, run * one, run)
    return factors


def xor_order(blocks, place):
    for bit in bits_of(len(blocks)):
        flip = (place & bit) != 0
        blocks = [jnp.where(flip, blocks[q ^ bit], blocks[q]) for q in range(len(blocks))]
    return blocks


def share_all(x, axis):
    count = lax.axis_size(axis)
    held = {0: x}
    for bit in bits_of(count):
        held.update({q ^ bit: swap_by(held[q], axis, bit) for q in list(held)})
    return [held[q] for q in range(count)]


def columns(x, count, dim):
    return jnp.split(x, count, axis=dim)


def from_later(keep_all, head, axis):
    count = lax.axis_size(axis)

    def shift(x, d):
        return lax.ppermute(x, axis, [(k, k - d) for k in range(d, count)])

    keep_span = shift(keep_all, 1)
    carry = shift(head, 1)
    d = 1
    while d < count:
        carry = carry + keep_span * shift(carry, d)
        if 2 * d < count:
            keep_span = keep_span * shift(keep_span, d)
        d *= 2
    return carry


def gelu_pair(values):
    result, pullback = jax.vjp(jax.nn.gelu, values)
    return (result, pullback(jnp.ones_like(values))[0])


def gate_maps(conv_out, weights):
    rows_here = conv_out.shape[0]
    blocked = conv_out.reshape(rows_here, weights.shape[0], weights.shape[1])
    mapped = jnp.einsum("tbi,bij->tbj", blocked, weights, preferred_element_type=jnp.float32)
    return mapped.reshape(rows_here, -1)


def gate_maps_back(grad_values, weights):
    rows_here = grad_values.shape[0]
    blocked = grad_values.reshape(rows_here, weights.shape[0], weights.shape[2])
    mapped = jnp.einsum(
        "tbj,bij->tbi", blocked, weights.astype(jnp.float32), precision=lax.Precision.HIGHEST
    )
    return mapped.reshape(rows_here, -1)


def norm_slope(spread):
    tiny_side = spread < SERIES_EDGE
    denominator = jnp.where(tiny_side, 1.0, -jnp.expm1(-spread))
    series_ratio = jnp.where(tiny_side, 1.0 + 0.5 * spread, spread / denominator)
    return 0.5 * jnp.sqrt(spread * series_ratio)


def reverse_linear(factors, term_values):
    rows, width = term_values.shape

    def kernel(factor_ref, term_ref, out_ref):
        def one(turn, state):
            at = pl.ds(rows - 1 - turn, 1)
            state = term_ref[at] + factor_ref[at] * state
            out_ref[at] = state
            return state

        lax.fori_loop(0, rows, one, jnp.zeros((1, width), jnp.float32), unroll=8)

    return pl.pallas_call(
        kernel, out_shape=jax.ShapeDtypeStruct((rows, width), jnp.float32), name="reverse_linear"
    )(factors, term_values)


def per_device(
    cotangent,
    residual,
    norm_gain,
    route_ids,
    route_weights,
    expert_gate,
    expert_up,
    expert_down,
    out_proj,
    conv_out,
    branch_gate,
    prev_state,
    decay_param,
    rate_map,
    input_map,
):
    tok_rows, model_width = residual.shape
    sp_count = lax.axis_size("sp")
    tp_count = lax.axis_size("tp")
    local_experts = expert_gate.shape[0]
    experts_all = local_experts * sp_count
    capacity = 4 * tok_rows // experts_all
    slot_total = experts_all * capacity
    sp_place = lax.axis_index("sp")
    tp_place = lax.axis_index("tp")
    part_cols = model_width // tp_count
    res_values = residual.astype(jnp.float32)
    inv_rms = lax.rsqrt(jnp.mean(res_values * res_values, axis=1, keepdims=True) + NORM_EPS)
    owner = jnp.arange(sp_count, dtype=jnp.int32)
    if is_direct(sp_count):
        owner = owner ^ sp_place
    expert_of = (
        owner[:, None] * local_experts + jnp.arange(local_experts, dtype=jnp.int32)[None, :]
    ).reshape(experts_all, 1)
    hits0 = expert_of == route_ids[:, 0][None, :]
    hits1 = expert_of == route_ids[:, 1][None, :]
    hits = hits0 | hits1
    before = jnp.arange(tok_rows)[:, None] < jnp.arange(tok_rows)[None, :]
    rank = jnp.dot(
        hits.astype(jnp.bfloat16), before.astype(jnp.bfloat16), preferred_element_type=jnp.float32
    ).astype(jnp.int32)
    slot_rank = jnp.where(hits, rank, -1)
    pick_mask = slot_rank[:, None, :] == jnp.arange(capacity, dtype=jnp.int32)[None, :, None]
    pick = pick_mask.astype(jnp.bfloat16).reshape(slot_total, tok_rows)
    pair_weight = jnp.where(hits0, route_weights[:, 0][None, :], route_weights[:, 1][None, :])
    slot_weight = jnp.sum(jnp.where(pick_mask, pair_weight[:, None, :], 0.0), axis=2).reshape(
        slot_total, 1
    )
    col_start = tp_place * part_cols
    res_part = lax.dynamic_slice_in_dim(residual, col_start, part_cols, 1).astype(jnp.float32)
    gain_part = lax.dynamic_slice_in_dim(norm_gain, col_start, part_cols, 0)
    rows_own = (res_part * inv_rms * gain_part[None, :]).astype(jnp.bfloat16)
    cot_own = lax.dynamic_slice_in_dim(cotangent, col_start, part_cols, 1)
    rows_send = jnp.dot(pick, rows_own, preferred_element_type=jnp.float32).astype(jnp.bfloat16)
    cot_send = (
        jnp.dot(pick, cot_own, preferred_element_type=jnp.float32) * slot_weight
    ).astype(jnp.bfloat16)

    def dispatch(rows):
        blocks = exchange(rows.reshape(sp_count, local_experts, capacity, part_cols), "sp")
        blocks = jnp.transpose(blocks, (1, 0, 2, 3))
        blocks = blocks.reshape(local_experts, sp_count * capacity, part_cols)
        return share_all(blocks, "tp")

    rows_in = dispatch(rows_send)
    cot_in = dispatch(cot_send)
    gate_w = xor_order(columns(expert_gate, tp_count, 1), tp_place)
    up_w = xor_order(columns(expert_up, tp_count, 1), tp_place)
    down_w = xor_order(columns(expert_down, tp_count, 2), tp_place)

    def total(form, lefts, rights):
        out = None
        for one, other in zip(lefts, rights):
            term = jnp.einsum(form, one, other, preferred_element_type=jnp.float32)
            out = term if out is None else out + term
        return out

    gate_pre = total("erd,edf->erf", rows_in, gate_w)
    up_pre = total("erd,edf->erf", rows_in, up_w)
    gate_sig = jax.nn.sigmoid(gate_pre)
    gate_act = gate_pre * gate_sig
    hidden = (gate_act * up_pre).astype(jnp.bfloat16)
    d_hidden = total("erd,efd->erf", cot_in, down_w)
    rate_gate = jax.nn.sigmoid(gate_maps(conv_out, rate_map))
    input_gate = jax.nn.sigmoid(gate_maps(conv_out, input_map))
    soft_decay = jax.nn.softplus(-decay_param)
    log_keep = -RATE_SCALE * rate_gate * soft_decay[None, :]
    keep_rate = jnp.exp(log_keep)
    spread = -2.0 * log_keep
    norm_term = jnp.sqrt(-jnp.expm1(-spread))
    conv_values = conv_out.astype(jnp.float32)
    prev_values = prev_state.astype(jnp.float32)
    state_now = keep_rate * prev_values + norm_term * input_gate * conv_values
    gelu_value, gelu_slope = gelu_pair(branch_gate.astype(jnp.float32))
    branch_out = (state_now * gelu_value).astype(jnp.bfloat16)
    block_keep = jnp.exp(jnp.sum(log_keep, axis=0))
    branch_out, _ = lax.optimization_barrier((branch_out, cot_in[0][:, :8, :128]))
    if is_direct(sp_count):
        tail_rows = 16
        branch_ext = with_tail(branch_out, three_pieces(block_keep), tail_rows)
        branch_all = [branch_ext] + [swap_by(branch_ext, "sp", j) for j in range(1, sp_count)]
        spans = [sum_pieces(one[tok_rows : tok_rows + 3]) for one in branch_all]
        factors = xor_order(later_factors(xor_order(spans, sp_place), sp_place), sp_place)
        d_hidden, branch_all = lax.optimization_barrier((d_hidden, branch_all))
    d_up = (d_hidden * gate_act).astype(jnp.bfloat16)
    d_gate = (d_hidden * up_pre * gate_sig * (1.0 + gate_pre * (1.0 - gate_sig))).astype(
        jnp.bfloat16
    )

    def back_term(q):
        return jnp.einsum(
            "erf,edf->erd", d_gate, gate_w[q], preferred_element_type=jnp.float32
        ) + jnp.einsum("erf,edf->erd", d_up, up_w[q], preferred_element_type=jnp.float32)

    back = {q: back_term(q) for q in reversed(range(tp_count))}
    for bit in reversed(bits_of(tp_count)):
        if bit == bits_of(tp_count)[0]:
            sent = back[bit]
        keep = [q for q in back if not q & bit]
        moved = {q: swap_by(back[q ^ bit].astype(jnp.bfloat16), "tp", bit) for q in keep}
        back = {q: back[q] + moved[q].astype(jnp.float32) for q in keep}
    summed = back[0].astype(jnp.bfloat16)
    summed = jnp.transpose(
        summed.reshape(local_experts, sp_count, capacity, part_cols), (1, 0, 2, 3)
    )
    returned = exchange(summed, "sp").reshape(slot_total, part_cols)
    normed_part = lax.dot_general(
        pick, returned, (((0,), (0,)), ((), ())), preferred_element_type=jnp.float32
    )
    d_normed = jnp.concatenate(
        xor_order(share_all(normed_part.astype(jnp.bfloat16), "tp"), tp_place), axis=1
    ).astype(jnp.float32)

    hidden, d_gate, d_up, _ = lax.optimization_barrier(
        (hidden, d_gate, d_up, sent[:, :8, :128])
    )

    def outer(form, lefts, rights, dim):
        parts = [
            jnp.einsum(form, one, other, preferred_element_type=jnp.float32)
            for one, other in zip(lefts, rights)
        ]
        return jnp.concatenate(xor_order(parts, tp_place), axis=dim)

    grad_down = outer("erf,erd->efd", [hidden] * tp_count, cot_in, 2)
    grad_gate = outer("erd,erf->edf", rows_in, [d_gate] * tp_count, 1)
    grad_up = outer("erd,erf->edf", rows_in, [d_up] * tp_count, 1)
    weighted = norm_gain[None, :] * d_normed
    cubed = inv_rms * inv_rms * inv_rms
    d_mix = (
        cotangent.astype(jnp.float32)
        + inv_rms * weighted
        - res_values * cubed * jnp.mean(res_values * weighted, axis=1, keepdims=True)
    ).astype(jnp.bfloat16)
    d_branch = jnp.dot(d_mix, out_proj, preferred_element_type=jnp.float32)
    next_keep = jnp.concatenate([keep_rate[1:], jnp.zeros_like(keep_rate[:1])], axis=0)
    local_grad = reverse_linear(next_keep, d_branch * gelu_value)
    next_log = jnp.concatenate([log_keep[1:], jnp.zeros_like(log_keep[:1])], axis=0)
    tail_keep = jnp.exp(jnp.flip(jnp.cumsum(jnp.flip(next_log, 0), axis=0), 0))
    head_term = keep_rate[0] * local_grad[0]

    if is_direct(sp_count):
        head_rows = three_pieces(head_term)
        head_ext = jnp.pad(head_rows, ((0, tail_rows - head_rows.shape[0]), (0, 0)))
        mix_send = deal_columns(d_mix, head_ext, sp_place, sp_count)
        mix_all = [mix_send[0]] + [swap_by(mix_send[j], "sp", j) for j in range(1, sp_count)]
        carried = sum(
            factors[j] * sum_pieces(mix_all[j][tok_rows : tok_rows + 3])
            for j in range(1, sp_count)
        )
        grad_out_proj = sum_outer(mix_all, branch_all, tok_rows)
    else:
        branch_all = lax.all_gather(branch_out, "sp")
        mix_all = exchange(jnp.stack(columns(d_mix, sp_count, 1)), "sp")
        grad_out_proj = lax.dot_general(
            mix_all.reshape(sp_count * tok_rows, -1),
            branch_all.reshape(sp_count * tok_rows, -1),
            (((0,), (0,)), ((), ())),
            preferred_element_type=jnp.float32,
        )
        carried = from_later(block_keep, head_term, "sp")
    state_grad = local_grad + tail_keep * carried[None, :]
    grad_branch_gate = d_branch * state_now * gelu_slope
    keep_grad = state_grad * prev_values * keep_rate
    inner_input = input_gate * conv_values
    rate_back = keep_grad * (-RATE_SCALE * soft_decay[None, :]) * rate_gate * (1.0 - rate_gate)
    rate_back = rate_back + state_grad * inner_input * keep_rate * keep_rate * (
        1.0 - rate_gate
    ) * norm_slope(spread)
    input_back = state_grad * norm_term * conv_values * input_gate * (1.0 - input_gate)
    grad_conv_out = (
        state_grad * norm_term * input_gate
        + gate_maps_back(rate_back, rate_map)
        + gate_maps_back(input_back, input_map)
    )
    return (grad_gate, grad_up, grad_down, grad_out_proj, grad_conv_out, grad_branch_gate)


def solution(mesh):
    in_specs = (
        P("sp", None),
        P("sp", None),
        P(),
        P("sp", None),
        P("sp", None),
        P("sp", None, "tp"),
        P("sp", None, "tp"),
        P("sp", "tp", None),
        P(None, "tp"),
        P("sp", "tp"),
        P("sp", "tp"),
        P("sp", "tp"),
        P("tp"),
        P("tp", None, None),
        P("tp", None, None),
    )
    out_specs = (
        P("sp", None, "tp"),
        P("sp", None, "tp"),
        P("sp", "tp", None),
        P("sp", "tp"),
        P("sp", "tp"),
        P("sp", "tp"),
    )
    return jax.shard_map(
        per_device, mesh=mesh, in_specs=in_specs, out_specs=out_specs, check_vma=False
    )
```
